32 devices in a mesh: fs: 16 (over z, y, x), tp: 2 (over core).
Axes of the slice: x: 2, y: 2, z: 4, core: 2. Of those that a mesh axis runs over, the one named last changes fastest.
Arguments:
- late_input: bfloat16 [2048, 2048], P('fs', 'tp'), may hold values from -6 to 6
- up_weight: bfloat16 [2048, 4096], P('tp', 'fs'), may hold values from -0.125 to 0.125
- down_weight: bfloat16 [4096, 2048], P('fs', 'tp'), may hold values from -0.09375 to 0.09375
- early_input: bfloat16 [2048, 2048], P('fs', 'tp'), may hold values from -6 to 6
- early_pre: bfloat16 [2048, 4096], P('fs'), may hold values from -6 to 6
- cotangent: bfloat16 [2048, 2048], P('fs', 'tp'), may hold values from -6 to 6
- up_sum: float32 [2048, 4096], P('tp', 'fs'), may hold values from -24 to 24
- down_sum: float32 [4096, 2048], P('fs', 'tp'), may hold values from -24 to 24
Outputs:
- late_pre: bfloat16 [2048, 4096], P('fs')
- late_out: bfloat16 [2048, 2048], P('fs', 'tp')
- input_grad: bfloat16 [2048, 2048], P('fs', 'tp')
- up_total: float32 [2048, 4096], P('tp', 'fs')
- down_total: float32 [4096, 2048], P('fs', 'tp')
The draws below stay inside these ranges and needn't reach their ends.
All inputs are finite; a program needn't handle non-finite values.
Results may differ from the reference program's by a relative error of at most 0.025.
Values may be sent and summed in bfloat16 or wider, within the bound.
No kernel may reach another device: no remote copies, remote signals or barrier semaphores. Data moves between devices by JAX's collectives and lax.ppermute only.
A program may use at most 128 MiB of HBM per device.

```python
import jax
import jax.numpy as jnp
from jax import lax

D = 2048
FF = 4096
TOKENS = 2048
DBLK = 1024
N_TP = 2


def spiked(drawn, own_key, source, target, parts, factor):
    owner, partner = [(jnp.arange(drawn.shape[axis_at]) // (drawn.shape[axis_at] // parts)).reshape([-1 if axis == axis_at else 1 for axis in range(drawn.ndim)]) for axis_at in (source, target)]
    chosen = jax.random.permutation(own_key, parts)[partner]
    strong = (owner == chosen) | (owner == (partner + parts // 2) % parts)
    return jnp.where(strong, factor * drawn, drawn)


def steps_of(key, shape, split, smallest, largest):
    def one(position, shards_of):
        draws = jax.random.uniform(jax.random.fold_in(jax.random.fold_in(key, 6), position), (shards_of,), jnp.float32, smallest / len(split), largest / len(split))
        return jnp.repeat(jnp.exp(draws), shape[position] // shards_of).reshape((-1,) + (1,) * (len(shape) - position - 1))

    factor_of = one(*split[0])
    for cut in split[1:]:
        factor_of = factor_of * one(*cut)
    return factor_of


def centred(rng, shape, width, reach, split=(), held_as=jnp.bfloat16):
    loudness = steps_of(rng, shape, split, -0.22, 0.18) if split else 1.0
    values = jax.random.normal(rng, shape, jnp.float32) * width * loudness
    return jnp.minimum(jnp.maximum(values, -reach), reach).astype(held_as)


def bell_draw_with(key, shape, width, bound, pieces, heavy, held_as=jnp.bfloat16):
    values = width * jax.random.normal(key, shape, jnp.float32)
    if pieces:
        values = values * steps_of(key, shape, pieces, -0.22, 0.18)
    return jnp.clip(spiked(values, jax.random.fold_in(key, 3), *heavy), -bound, bound).astype(held_as)


def setup_inputs(seed: int = 0) -> dict:
    arg_keys = jax.random.split(jax.random.key(seed), 9)
    return {
        "late_input": centred(arg_keys[0], (TOKENS, D), 1.0, 6.0, ((0, 16), (1, 2))),
        "up_weight": centred(arg_keys[1], (D, FF), D ** -0.5, 0.125, ((0, 2), (1, 16))),
        "down_weight": centred(arg_keys[2], (FF, D), FF ** -0.5, 0.09375, ((0, 16), (1, 2))),
        "early_input": centred(arg_keys[3], (TOKENS, D), 1.0, 6.0, ((0, 16), (1, 2))),
        "early_pre": centred(arg_keys[4], (TOKENS, FF), 1.0, 6.0, ((0, 16),)),
        "cotangent": bell_draw_with(arg_keys[5], (TOKENS, D), 1.0, 6.0, ((0, 16), (1, 2)), (0, 1, 16, 2.0)),
        "up_sum": centred(arg_keys[6], (D, FF), 4.0, 24.0, ((0, 2), (1, 16)), jnp.float32),
        "down_sum": centred(arg_keys[7], (FF, D), 4.0, 24.0, ((0, 16), (1, 2)), jnp.float32),
    }


def block_sum(left, right):
    total = jnp.zeros((left.shape[0], right.shape[1]), jnp.float32)
    for block in range(N_TP):
        lower = block * DBLK
        partial_value = jnp.dot(left[:, lower:lower + DBLK], right[lower:lower + DBLK, :], preferred_element_type=jnp.float32)
        partial_value = lax.optimization_barrier(partial_value.astype(jnp.bfloat16))
        total = total + partial_value.astype(jnp.float32)
    return total


def reference(late_input, up_weight, down_weight, early_input, early_pre, cotangent, up_sum, down_sum):
    late_pre = block_sum(late_input, up_weight).astype(jnp.bfloat16)
    late_hidden = jnp.square(jax.nn.relu(late_pre.astype(jnp.float32))).astype(jnp.bfloat16)
    late_out = jnp.dot(late_hidden, down_weight, preferred_element_type=jnp.float32).astype(jnp.bfloat16)
    early_float = early_pre.astype(jnp.float32)
    early_hidden = jnp.square(jax.nn.relu(early_float)).astype(jnp.bfloat16)
    hidden_grad = block_sum(cotangent, down_weight.T)
    pre_grad = (hidden_grad * 2.0 * jax.nn.relu(early_float)).astype(jnp.bfloat16)
    input_grad = jnp.dot(pre_grad, up_weight.T, preferred_element_type=jnp.float32).astype(jnp.bfloat16)
    up_total = up_sum + jnp.dot(early_input.T, pre_grad, preferred_element_type=jnp.float32)
    down_total = down_sum + jnp.dot(early_hidden.T, cotangent, preferred_element_type=jnp.float32)
    return late_pre, late_out, input_grad, up_total, down_total
```

```python
import functools

import jax
import jax.numpy as jnp
from jax import lax
from jax.experimental import pallas as pl
from jax.experimental.pallas import tpu as pltpu
from jax.sharding import PartitionSpec as P

F32 = jnp.float32
BF16 = jnp.bfloat16


def dot_nn(left, right):
    return lax.dot_general(left, right, (((1,), (0,)), ((), ())), preferred_element_type=F32)


def dot_tn(left, right):
    return lax.dot_general(left, right, (((0,), (0,)), ((), ())), preferred_element_type=F32)


def dot_nt(left, right):
    return lax.dot_general(left, right, (((1,), (1,)), ((), ())), preferred_element_type=F32)


def split_bits(size):
    count = size.bit_length() - 1
    assert 1 << count == size
    tokens = [bit for bit in range(count) if bit % 4 in (0, 3)]
    hidden = [bit for bit in range(count) if bit % 4 in (1, 2)]
    return tokens[::-1], hidden[::-1]


def offset_of(bits, rel):
    return sum(1 << bit for place, bit in enumerate(bits) if rel >> place & 1)


class Links:
    def __init__(self, fs, tp):
        self.fs, self.tp = fs, tp

    def send(self, value, offset):
        return lax.ppermute(value, "fs", [(i, i ^ offset) for i in range(self.fs)])

    def gather(self, own, bits):
        blocks = [own]
        for bit in bits:
            blocks = blocks + [self.send(block, 1 << bit) for block in blocks]
        return blocks

    def exchange(self, blocks, bits):
        return [blocks[0]] + [
            self.send(block, offset_of(bits, rel)) for rel, block in enumerate(blocks) if rel
        ]

    def reduce_scatter(self, blocks, bits):
        blocks = list(blocks)
        for bit in bits[::-1]:
            half = len(blocks) // 2
            received = [None] * half
            for place in range(half)[::-1]:
                received[place] = self.send(blocks[half + place].astype(BF16), 1 << bit)
            blocks = [mine + other.astype(F32) for mine, other in zip(blocks[:half], received)]
        return blocks[0]

    def sum_parts(self, part):
        if self.tp == 2:
            other = lax.ppermute(part, "tp", [(0, 1), (1, 0)])
            return part.astype(F32) + other.astype(F32)
        return lax.psum(part.astype(F32), "tp").astype(F32)


def reorder_kernel(count, width, groups, pos_ref, x_ref, *out_refs):
    pos = pos_ref[0]
    for out_ref, members in zip(out_refs, groups):
        for place, rel in enumerate(members):
            start = pl.multiple_of(lax.bitwise_xor(pos, jnp.int32(rel)) * width, width)
            out_ref[:, place * width:(place + 1) * width] = x_ref[:, pl.ds(start, width)]


def unorder_kernel(count, width, groups, pos_ref, *refs):
    out_ref = refs[-1]
    pos = pos_ref[0]
    for in_ref, members in zip(refs[:-1], groups):
        for place, rel in enumerate(members):
            start = pl.multiple_of(lax.bitwise_xor(pos, jnp.int32(rel)) * width, width)
            out_ref[:, pl.ds(start, width)] = in_ref[:, place * width:(place + 1) * width]


def swap_bits(value, pos, count, width):
    rows = value.shape[0]
    bit = 1
    while bit < count:
        view = value.reshape(rows, count // (2 * bit), 2, bit * width)
        value = jnp.where((pos & bit) != 0, view[:, :, ::-1], view).reshape(rows, count * width)
        bit *= 2
    return value


def to_relative(value, pos, count, width, groups):
    rows = value.shape[0]
    if width % 128:
        value = swap_bits(value, pos, count, width)
        return [
            jnp.concatenate([value[:, rel * width:(rel + 1) * width] for rel in members], axis=1)
            for members in groups
        ]
    return pl.pallas_call(
        functools.partial(reorder_kernel, count, width, groups),
        out_shape=[jax.ShapeDtypeStruct((rows, width * len(m)), value.dtype) for m in groups],
        in_specs=[
            pl.BlockSpec(memory_space=pltpu.SMEM),
            pl.BlockSpec(memory_space=pltpu.VMEM),
        ],
        out_specs=[pl.BlockSpec(memory_space=pltpu.VMEM) for _ in groups],
        name="to_relative",
    )(pos[None], value)


def from_relative(values, pos, count, width, groups):
    rows = values[0].shape[0]
    if width % 128:
        pieces = [None] * count
        for value, members in zip(values, groups):
            for place, rel in enumerate(members):
                pieces[rel] = value[:, place * width:(place + 1) * width]
        return swap_bits(jnp.concatenate(pieces, axis=1), pos, count, width)
    return pl.pallas_call(
        functools.partial(unorder_kernel, count, width, groups),
        out_shape=jax.ShapeDtypeStruct((rows, width * count), values[0].dtype),
        in_specs=[pl.BlockSpec(memory_space=pltpu.SMEM)]
        + [pl.BlockSpec(memory_space=pltpu.VMEM) for _ in values],
        out_specs=pl.BlockSpec(memory_space=pltpu.VMEM),
        name="from_relative",
    )(pos[None], *values)


def body(fs, tp, late_input, up_weight, down_weight, early_input, early_pre, cotangent, up_sum, down_sum):
    links = Links(fs, tp)
    t_bits, h_bits = split_bits(fs)
    n_t, n_h = 1 << len(t_bits), 1 << len(h_bits)
    pos = lax.axis_index("fs").astype(jnp.int32)
    core = lax.axis_index("tp").astype(jnp.int32)
    rows = late_input.shape[0]
    width = up_weight.shape[1]
    groups = [[offset_of(t_bits, t) ^ offset_of(h_bits, h) for h in range(n_h)] for t in range(n_t)]

    share = rows // 2 if tp == 2 else rows
    mine = lax.dynamic_slice_in_dim(early_pre, core * share, share, 0) if tp == 2 else early_pre
    pre_out = to_relative(mine, pos, fs, width, groups)
    pre_in = links.exchange(pre_out, t_bits)
    pre_half = jnp.concatenate(pre_in, axis=0)

    cot_blocks = links.gather(cotangent, t_bits)
    down_blocks = links.gather(down_weight, h_bits)
    late_blocks = links.gather(late_input, t_bits)
    up_blocks = links.gather(up_weight, h_bits)
    early_blocks = links.gather(early_input, t_bits)

    if tp == 2:
        pre_other = lax.ppermute(pre_half, "tp", [(0, 1), (1, 0)])
        a = pre_half.reshape(n_t, share, n_h * width)
        b = pre_other.reshape(n_t, share, n_h * width)
        first = jnp.where(core == 0, a, b)
        second = jnp.where(core == 0, b, a)
        pre = jnp.concatenate([first, second], axis=1).reshape(n_t * rows, n_h * width)
    else:
        pre = pre_half
    pre_relu = jax.nn.relu(pre.astype(F32))
    early_hidden = jnp.square(pre_relu).astype(BF16)

    cot = jnp.concatenate(cot_blocks, axis=0)
    down = jnp.concatenate(down_blocks, axis=0)
    late = jnp.concatenate(late_blocks, axis=0)
    up = jnp.concatenate(up_blocks, axis=1)
    early = jnp.concatenate(early_blocks, axis=0)

    grad_part = dot_nt(cot, down).astype(BF16)
    hidden_grad = links.sum_parts(grad_part)
    pre_grad = (hidden_grad * 2.0 * pre_relu).astype(BF16)

    down_grad = [
        dot_tn(early_hidden[:, h * width:(h + 1) * width], cot) for h in range(n_h)
    ]
    down_total = down_sum + links.reduce_scatter(down_grad, h_bits)

    late_part = dot_nn(late, up).astype(BF16)
    late_pre = links.sum_parts(late_part).astype(BF16)
    late_hidden = jnp.square(jax.nn.relu(late_pre.astype(F32))).astype(BF16)

    late_terms = dot_nn(late_hidden, down)
    late_out = links.reduce_scatter(
        [late_terms[t * rows:(t + 1) * rows] for t in range(n_t)], t_bits
    ).astype(BF16)
    input_terms = dot_nt(pre_grad, up)
    input_grad = links.reduce_scatter(
        [input_terms[t * rows:(t + 1) * rows] for t in range(n_t)], t_bits
    ).astype(BF16)

    up_grad = [
        dot_tn(early, pre_grad[:, h * width:(h + 1) * width]) for h in range(n_h)
    ]
    up_total = up_sum + links.reduce_scatter(up_grad, h_bits)

    late_view = late_pre.reshape(n_t, rows, n_h * width)
    if tp == 2:
        late_view = lax.dynamic_slice_in_dim(late_view, core * share, share, 1)
    back = links.exchange([late_view[t] for t in range(n_t)], t_bits)
    part = from_relative(back, pos, fs, width, groups)
    if tp == 2:
        other = lax.ppermute(part, "tp", [(0, 1), (1, 0)])
        late_out_pre = jnp.concatenate(
            [jnp.where(core == 0, part, other), jnp.where(core == 0, other, part)], axis=0
        )
    else:
        late_out_pre = part
    return (late_out_pre, late_out, input_grad, up_total, down_total)


def solution(mesh):
    in_specs = (
        P("fs", "tp"),
        P("tp", "fs"),
        P("fs", "tp"),
        P("fs", "tp"),
        P("fs", None),
        P("fs", "tp"),
        P("tp", "fs"),
        P("fs", "tp"),
    )
    out_specs = (P("fs", None), P("fs", "tp"), P("fs", "tp"), P("tp", "fs"), P("fs", "tp"))
    return jax.shard_map(
        functools.partial(body, mesh.shape["fs"], mesh.shape["tp"]),
        mesh=mesh, in_specs=in_specs, out_specs=out_specs, check_vma=False,
    )
```
